32 devices in a mesh: sp: 16 (over z, y, x), tp: 2 (over core).
Axes of the slice: x: 2, y: 2, z: 4, core: 2. Of those that a mesh axis runs over, the one named last changes fastest.
Arguments:
- prompt: bfloat16 [8, 1024, 2048], P(None, 'sp'), may hold values from -6 to 6
- keep_scale: float32 [8, 1024], P(None, 'sp'), may hold values from 0.25 to 1
- new_token: bfloat16 [8, 2048], P(None, 'tp'), may hold values from -6 to 6
- w_query: bfloat16 [2048, 1024], P(None, 'tp'), may hold values from -0.125 to 0.125
- w_forget: bfloat16 [2048, 1024], P(None, 'tp'), may hold values from -0.125 to 0.125
- w_value: bfloat16 [2048, 1024], P(None, 'tp'), may hold values from -2.109375 to 2.109375
- w_outgate: bfloat16 [2048, 1024], P(None, 'tp'), may hold values from -0.125 to 0.125
- floor_gap: float32 [1024], P('tp'), may hold values from 0 to 0.06
- norm_gain: float32 [128], replicated, may hold values from 0.1 to 1.9
Outputs:
- state_cache: bfloat16 [8, 1024, 128], P('tp', 'sp')
- first_read: bfloat16 [8, 1024], P(None, 'tp')
The draws below stay inside these ranges and needn't reach their ends.
All inputs are finite; a program needn't handle non-finite values.
Results may differ from the reference program's by a relative error of at most 0.0022.
The reference program's roundings to bfloat16 on the way (of `values` and `new_value`) count: a program that leaves them out, or rounds other values in their place, can miss the bound.
Values may be sent and summed in bfloat16 or wider, within the bound.
A program may use at most 64 MiB of HBM per device.

```python
import math
import jax
import jax.numpy as jnp
from jax import lax

D = 2048
HEADS = 8
HEAD_DIM = 128
MIX_WIDTH = 1024
PROMPT_COUNT = 8
TOK_SEQ = 64
PROMPT_LENGTH = 1024


def draw_keep_scale(key, part):
    key_rate = jax.random.fold_in(key, 11)
    key_positions = jax.random.fold_in(key, 12)
    key_depth = jax.random.fold_in(key, 13)
    blocks = PROMPT_LENGTH // TOK_SEQ
    block_rate = jnp.exp(jax.random.uniform(key_rate, (PROMPT_COUNT, blocks, 1), minval=math.log(0.4), maxval=math.log(1.6))) / PROMPT_LENGTH
    steady = jnp.broadcast_to(jnp.exp(-block_rate), (PROMPT_COUNT, blocks, TOK_SEQ)).reshape(PROMPT_COUNT, PROMPT_LENGTH)
    spike_positions = jax.random.randint(key_positions, (PROMPT_COUNT, 2), 0, PROMPT_LENGTH)
    spike_match = jnp.arange(PROMPT_LENGTH, dtype=jnp.int32)[None, None, :] == spike_positions[:, :, None]
    intensity = jax.random.uniform(key_depth, (PROMPT_COUNT, 2, 1), minval=0.55, maxval=0.8)
    multiplier = jnp.prod(jnp.where(spike_match, intensity, 1.0), axis=1)
    return (steady * multiplier).astype(jnp.float32)


def draw_floor_gap(key, part):
    key_order = jax.random.fold_in(key, 21)
    key_fast = jax.random.fold_in(key, 22)
    key_slow = jax.random.fold_in(key, 23)
    head_order = jax.random.permutation(key_order, HEADS)
    fast_count = HEADS // 2
    fast_head = head_order < fast_count
    fast_gap = jnp.exp(jax.random.uniform(key_fast, (HEADS, HEAD_DIM), minval=math.log(0.02), maxval=math.log(0.06)))
    slow_gap = jnp.exp(jax.random.uniform(key_slow, (HEADS, HEAD_DIM), minval=math.log(0.2), maxval=0.0)) / PROMPT_LENGTH
    return jnp.where(fast_head[:, None], fast_gap, slow_gap).reshape(HEADS * HEAD_DIM).astype(jnp.float32)


def levels(key, extent, split, least, largest):
    factor_of = 1.0
    for position, parts in split:
        steps = jax.random.uniform(jax.random.fold_in(jax.random.fold_in(key, 6), position), (parts,), jnp.float32, least / len(split), largest / len(split))
        factor_of = factor_of * jnp.repeat(jnp.exp(steps), extent[position] // parts).reshape((-1,) + (1,) * (len(extent) - 1 - position))
    return factor_of


def normal_values(key, dims, deviation, most, split=(), kind=jnp.bfloat16):
    values = jax.random.normal(key, dims, jnp.float32) * deviation
    if len(split) > 0:
        values = levels(key, dims, split, -0.22, 0.18) * values
    return jnp.clip(values, min=-most, max=most).astype(kind)


def setup_inputs(seed: int = 0) -> dict:
    splits = jax.random.split(jax.random.key(seed), 10)
    return {
        "prompt": normal_values(splits[0], (PROMPT_COUNT, PROMPT_LENGTH, D), 1.0, 6.0, ((1, 16),)),
        "keep_scale": draw_keep_scale(jax.random.fold_in(splits[9], 71), 0),
        "new_token": normal_values(splits[2], (PROMPT_COUNT, D), 1.0, 6.0, ((1, 2),)),
        "w_query": normal_values(splits[3], (D, MIX_WIDTH), D ** -0.5, 0.125, ((1, 2),)),
        "w_forget": normal_values(splits[4], (D, MIX_WIDTH), D ** -0.5, 0.125, ((1, 2),)),
        "w_value": normal_values(splits[5], (D, MIX_WIDTH), (0.5 * PROMPT_LENGTH ** 0.5 * D ** -0.5), 2.109375, ((1, 2),)),
        "w_outgate": normal_values(splits[6], (D, MIX_WIDTH), D ** -0.5, 0.125, ((1, 2),)),
        "floor_gap": draw_floor_gap(jax.random.fold_in(splits[9], 71), 0),
        "norm_gain": jnp.clip(1.0 + 0.18 * jax.random.normal(splits[8], (HEAD_DIM,), jnp.float32), 0.1, 1.9),
    }


EPSILON = 1e-06

def reference(prompt, keep_scale, new_token, w_query, w_forget, w_value, w_outgate, floor_gap, norm_gain):
    floor_rows = floor_gap.reshape(HEADS, HEAD_DIM)

    def one_sequence(inputs):
        seq_rows, keep_row = inputs
        forget_pre = jnp.dot(seq_rows, w_forget, preferred_element_type=jnp.float32).reshape(PROMPT_LENGTH, HEADS, HEAD_DIM)
        values = jnp.dot(seq_rows, w_value, preferred_element_type=jnp.float32).astype(jnp.bfloat16)
        values = lax.optimization_barrier(values).astype(jnp.float32).reshape(PROMPT_LENGTH, HEADS, HEAD_DIM)
        forget_loss = floor_rows * (1.0 - jax.nn.sigmoid(forget_pre))
        keep_factor = keep_row[:, None, None]
        log_forget = jnp.log(keep_factor) + jnp.log1p(-forget_loss)
        input_gate = 1.0 - keep_factor + keep_factor * forget_loss
        later_log = lax.cumsum(log_forget, axis=0, reverse=True) - log_forget
        return jnp.einsum('thc,thv->hcv', input_gate * jnp.exp(later_log), values, precision=lax.Precision.HIGHEST)
    final_state = lax.map(one_sequence, (prompt, keep_scale))
    state_cache = final_state.transpose(1, 0, 2, 3).reshape(HEADS, PROMPT_COUNT * HEAD_DIM, HEAD_DIM).astype(jnp.bfloat16)
    shaped = (PROMPT_COUNT, HEADS, HEAD_DIM)
    query = jnp.dot(new_token, w_query, preferred_element_type=jnp.float32).reshape(shaped)
    new_forget = jnp.dot(new_token, w_forget, preferred_element_type=jnp.float32).reshape(shaped)
    new_gate = jnp.dot(new_token, w_outgate, preferred_element_type=jnp.float32).reshape(shaped)
    new_value = jnp.dot(new_token, w_value, preferred_element_type=jnp.float32).astype(jnp.bfloat16)
    new_value = lax.optimization_barrier(new_value).astype(jnp.float32).reshape(shaped)
    new_loss = floor_rows * (1.0 - jax.nn.sigmoid(new_forget))
    mixed = jnp.einsum('shc,shcv->shv', query * (1.0 - new_loss), final_state, precision=lax.Precision.HIGHEST)
    mixed = mixed + lax.optimization_barrier(jnp.sum(query * new_loss, axis=-1, keepdims=True)) * new_value
    normed = mixed * lax.rsqrt(lax.optimization_barrier(jnp.mean(mixed * mixed, axis=-1, keepdims=True)) + EPSILON)
    first_read = (normed * norm_gain * jax.nn.silu(new_gate)).reshape(PROMPT_COUNT, HEADS * HEAD_DIM).astype(jnp.bfloat16)
    return (state_cache, first_read)
```

```python
import functools

import jax
import jax.numpy as jnp
from jax import lax
from jax.experimental import pallas as pl
from jax.experimental.pallas import tpu as pltpu
from jax.sharding import PartitionSpec as P

EPSILON = 1e-06
MESH = pl.DeviceIdType.MESH
F32 = jnp.float32
BF16 = jnp.bfloat16


def swap(mine, step, count):
    if count & (count - 1):
        return lax.rem(step - mine + 2 * count, count)
    total, bit = 0, 1
    while bit < count:
        total = total + bit * lax.rem(lax.rem(mine // bit, 2) + lax.rem(step // bit, 2), 2)
        bit *= 2
    return total


def pieces(x, count):
    out = []
    for _ in range(count):
        piece = x.astype(BF16)
        out.append(piece)
        x = x - piece.astype(F32)
    return out


def kernel(
    sizes,
    prompt, keep, token, w_query, w_forget, w_value, w_outgate, floor, gain,
    cache_out, read_out,
    blocks, keeps, tokens, wq, wf, wv, wo, weighted, values, logs, states, got_states, reads, sums,
    local_sem, direct_send, direct_recv, keep_send, keep_recv, fwd_send, fwd_recv,
    token_send, token_recv, log_send, log_recv, state_send, state_recv, read_send, read_recv,
):
    n, t, s_count, group, heads, head, rows = sizes
    me, core = lax.axis_index("sp"), lax.axis_index("tp")
    mine, place = me // group, lax.rem(me, group)
    model = prompt.shape[2]
    part = model // t
    positions = prompt.shape[1]
    width = heads * head

    def columns(c):
        return pl.ds(pl.multiple_of(c * part, part), part)

    def order(i):
        half = s_count // 2
        if s_count % 2:
            return i
        return 2 * lax.rem(half - i // 2, half) + lax.rem(i, 2)

    def peer(i):
        return swap(mine, order(i), s_count)

    local = [
        pltpu.make_async_copy(prompt.at[mine], blocks.at[mine], local_sem.at[0]),
        pltpu.make_async_copy(w_forget, wf, local_sem.at[1]),
        pltpu.make_async_copy(w_value, wv, local_sem.at[2]),
        pltpu.make_async_copy(w_query, wq, local_sem.at[3]),
        pltpu.make_async_copy(w_outgate, wo, local_sem.at[4]),
    ]

    barrier = pltpu.get_barrier_semaphore()
    for o in range(1, n):
        pl.semaphore_signal(barrier, inc=1, device_id=(lax.rem(me + o, n), core), device_id_type=MESH)
    for o in range(1, t):
        pl.semaphore_signal(barrier, inc=1, device_id=(me, lax.rem(core + o, t)), device_id_type=MESH)
    for copy in local:
        copy.start()
    pl.semaphore_wait(barrier, n - 1 + t - 1)

    def direct(i):
        to = peer(i)
        return pltpu.make_async_remote_copy(
            src_ref=prompt.at[to, :, columns(core)],
            dst_ref=blocks.at[mine, :, columns(core)],
            send_sem=direct_send.at[i], recv_sem=direct_recv.at[i],
            device_id=(to * group + place, core), device_id_type=MESH,
        )

    def direct_in(i):
        frm = peer(i)
        return pltpu.make_async_remote_copy(
            src_ref=prompt.at[frm, :, columns(core)],
            dst_ref=blocks.at[frm, :, columns(core)],
            send_sem=direct_send.at[i], recv_sem=direct_recv.at[i],
            device_id=(frm * group + place, core), device_id_type=MESH,
        )

    def keep_copy(i):
        to = peer(i)
        return pltpu.make_async_remote_copy(
            src_ref=keep, dst_ref=keeps.at[i],
            send_sem=keep_send.at[i], recv_sem=keep_recv.at[i],
            device_id=(to * group + place, core), device_id_type=MESH,
        )

    def forward(i, o):
        frm = peer(i)
        return pltpu.make_async_remote_copy(
            src_ref=blocks.at[frm, :, columns(core)],
            dst_ref=blocks.at[frm, :, columns(core)],
            send_sem=fwd_send.at[i, o], recv_sem=fwd_recv.at[i, o],
            device_id=(me, lax.rem(core + o, t)), device_id_type=MESH,
        )

    def forward_in(i, o):
        frm = peer(i)
        c = lax.rem(core - o + t, t)
        return pltpu.make_async_remote_copy(
            src_ref=blocks.at[frm, :, columns(c)],
            dst_ref=blocks.at[frm, :, columns(c)],
            send_sem=fwd_send.at[i, o], recv_sem=fwd_recv.at[i, o],
            device_id=(me, lax.rem(core + o, t)), device_id_type=MESH,
        )

    def token_copy(o, c):
        return pltpu.make_async_remote_copy(
            src_ref=token, dst_ref=tokens.at[c],
            send_sem=token_send.at[o], recv_sem=token_recv.at[o],
            device_id=(me, lax.rem(core + o, t)), device_id_type=MESH,
        )

    for i in range(1, s_count):
        keep_copy(i).start()
        direct(i).start()
    for o in range(1, t):
        token_copy(o, core).start()

    keeps[0] = keep[...]
    tokens[core] = token[...]
    floor_row = floor[...]

    def forget(j, i):
        pre = jnp.dot(blocks[j], wf[...], preferred_element_type=F32)
        loss = floor_row * (1.0 / (1.0 + jnp.exp(pre)))
        row = keeps[i, pl.ds(mine, 1), :]
        r = lax.broadcasted_iota(jnp.int32, (positions, positions), 0)
        c = lax.broadcasted_iota(jnp.int32, (positions, positions), 1)
        scale = jnp.sum(jnp.where(r == c, jnp.broadcast_to(row, (positions, positions)), 0.0), axis=1, keepdims=True)
        log_forget = jnp.log(scale) + jnp.log1p(-loss)
        gate = 1.0 - scale + scale * loss
        later = jnp.where(c > r, 1.0, 0.0).astype(BF16)
        inside = sum(jnp.dot(later, p, preferred_element_type=F32) for p in pieces(log_forget, 3))
        logs[0, pl.ds(j, 1), :] = inside[0:1] + log_forget[0:1]
        weighted[j] = gate * jnp.exp(inside)

    def value(j):
        values[j] = jnp.dot(blocks[j], wv[...], preferred_element_type=F32).astype(BF16)

    local[0].wait()
    local[1].wait()
    local[2].wait()
    forget(mine, 0)
    value(mine)

    local[3].wait()
    local[4].wait()
    for o in range(1, t):
        token_copy(o, lax.rem(core - o + t, t)).wait_recv()
    feature = jnp.concatenate([tokens[c] for c in range(t)], axis=1)
    query = jnp.dot(feature, wq[...], preferred_element_type=F32)
    new_forget = jnp.dot(feature, wf[...], preferred_element_type=F32)
    new_value = jnp.dot(feature, wv[...], preferred_element_type=F32).astype(BF16).astype(F32)
    new_gate = jnp.dot(feature, wo[...], preferred_element_type=F32)
    new_loss = floor_row * (1.0 / (1.0 + jnp.exp(new_forget)))
    read_weight = query * (1.0 - new_loss)
    own = query * new_loss
    silu = new_gate * (1.0 / (1.0 + jnp.exp(-new_gate)))
    sums[0] = own
    sums[1] = new_value
    sums[2] = silu
    seq = lax.broadcasted_iota(jnp.int32, read_weight.shape, 0)
    sums[3] = jnp.broadcast_to(
        jnp.sum(jnp.where(seq == mine, read_weight, 0.0), axis=0, keepdims=True), read_weight.shape
    )

    def arrive(i):
        direct_in(i).wait_recv()
        for o in range(1, t):
            forward(i, o).start()

    def ready(i):
        keep_copy(i).wait_recv()
        for o in range(1, t):
            forward_in(i, o).wait_recv()

    arrive(1)

    def step(i, carry):
        arrive(i)
        ready(i - 1)
        j = peer(i - 1)
        forget(j, i - 1)
        value(j)
        return carry

    lax.fori_loop(2, s_count, step, 0)
    last = s_count - 1
    ready(last)
    j = peer(last)
    forget(j, last)

    def log_copy(o):
        return pltpu.make_async_remote_copy(
            src_ref=logs.at[0], dst_ref=logs.at[o],
            send_sem=log_send.at[o], recv_sem=log_recv.at[o],
            device_id=(mine * group + lax.rem(place + o, group), core), device_id_type=MESH,
        )

    for o in range(1, group):
        log_copy(o).start()
    value(j)
    for o in range(1, group):
        log_copy(o).wait_recv()

    own_log = logs[0]
    total, beside = own_log, jnp.zeros_like(own_log)
    for o in range(1, group):
        other = logs[o]
        total = total + other
        beside = beside + jnp.where(lax.rem(place - o + group, group) > place, other, 0.0)
    suffix = jnp.zeros((1, width), F32)
    for b in reversed(range(s_count)):
        weighted[b] = weighted[b] * jnp.exp(suffix + beside[b : b + 1])
        suffix = suffix + total[b : b + 1]

    def state_copy(o):
        to = lax.rem(place + o, group)
        return pltpu.make_async_remote_copy(
            src_ref=states.at[:, pl.ds(pl.multiple_of(to * rows, rows), rows), :], dst_ref=got_states.at[o],
            send_sem=state_send.at[o], recv_sem=state_recv.at[o],
            device_id=(mine * group + to, core), device_id_type=MESH,
        )

    def read_copy(o, sender):
        return pltpu.make_async_remote_copy(
            src_ref=reads.at[sender], dst_ref=reads.at[sender],
            send_sem=read_send.at[o], recv_sem=read_recv.at[o],
            device_id=(lax.rem(me + o, n), core), device_id_type=MESH,
        )

    for h in range(heads):
        lanes = slice(h * head, (h + 1) * head)
        w = weighted[:, :, lanes].reshape(s_count * positions, head)
        v = values[:, :, lanes].reshape(s_count * positions, head)
        state = sum(
            lax.dot_general(p, v, (((0,), (0,)), ((), ())), preferred_element_type=F32) for p in pieces(w, 2)
        )
        states[h] = state
        part_read = jnp.dot(sums[3, :, lanes], state, preferred_element_type=F32, precision=lax.Precision.HIGHEST)
        reads[me, :, lanes] = part_read[0:1]

    for o in range(n - 1, 0, -1):
        read_copy(o, me).start()
    for o in range(1, group):
        state_copy(o).start()

    start = pl.multiple_of(place * rows, rows)
    for o in range(1, group):
        state_copy(o).wait_recv()
    final = states[:, pl.ds(start, rows), :]
    for o in range(1, group):
        final = final + got_states[o]
    cache_out[...] = final.astype(BF16)

    for o in range(1, n):
        read_copy(o, lax.rem(me - o + n, n)).wait_recv()
    for s in range(s_count):
        row = reads[s * group]
        for g in range(1, group):
            row = row + reads[s * group + g]
        sums[4, s : s + 1, :] = row
    for h in range(heads):
        lanes = slice(h * head, (h + 1) * head)
        mixed = sums[4, :, lanes] + jnp.sum(sums[0, :, lanes], axis=1, keepdims=True) * sums[1, :, lanes]
        normed = mixed * lax.rsqrt(jnp.mean(mixed * mixed, axis=1, keepdims=True) + EPSILON)
        read_out[:, lanes] = (normed * gain[...] * sums[2, :, lanes]).astype(BF16)

    for i in range(1, s_count):
        keep_copy(i).wait_send()
        direct(i).wait_send()
        for o in range(1, t):
            forward(i, o).wait_send()
    for o in range(1, t):
        token_copy(o, core).wait_send()
    for o in range(1, group):
        log_copy(o).wait_send()
        state_copy(o).wait_send()
    for o in range(1, n):
        read_copy(o, me).wait_send()


def per_device(prompt, keep_scale, new_token, w_query, w_forget, w_value, w_outgate, floor_gap, norm_gain):
    n, t = lax.axis_size("sp"), lax.axis_size("tp")
    s_count, positions, model = prompt.shape
    head = norm_gain.shape[0]
    width = w_forget.shape[1]
    heads = width // head
    group = n // s_count
    rows = head // group
    sizes = (n, t, s_count, group, heads, head, rows)
    dma = pltpu.SemaphoreType.DMA
    vmem = pl.BlockSpec(memory_space=pltpu.VMEM)
    hbm = pl.BlockSpec(memory_space=pl.ANY)
    return pl.pallas_call(
        functools.partial(kernel, sizes),
        out_shape=(
            jax.ShapeDtypeStruct((heads, rows, head), BF16),
            jax.ShapeDtypeStruct((s_count, width), BF16),
        ),
        in_specs=[hbm, vmem, vmem, hbm, hbm, hbm, hbm, vmem, vmem],
        out_specs=(vmem, vmem),
        scratch_shapes=[
            pltpu.VMEM((s_count, positions, model), BF16),
            pltpu.VMEM((s_count,) + keep_scale.shape, F32),
            pltpu.VMEM((t,) + new_token.shape, BF16),
            pltpu.VMEM((model, width), BF16),
            pltpu.VMEM((model, width), BF16),
            pltpu.VMEM((model, width), BF16),
            pltpu.VMEM((model, width), BF16),
            pltpu.VMEM((s_count, positions, width), F32),
            pltpu.VMEM((s_count, positions, width), BF16),
            pltpu.VMEM((group, s_count, width), F32),
            pltpu.VMEM((heads, head, head), F32),
            pltpu.VMEM((group, heads, rows, head), F32),
            pltpu.VMEM((n, 1, width), F32),
            pltpu.VMEM((5, s_count, width), F32),
            dma((5,)),
            dma((s_count,)), dma((s_count,)),
            dma((s_count,)), dma((s_count,)),
            dma((s_count, t)), dma((s_count, t)),
            dma((t,)), dma((t,)),
            dma((group,)), dma((group,)),
            dma((group,)), dma((group,)),
            dma((n,)), dma((n,)),
        ],
        compiler_params=pltpu.CompilerParams(collective_id=0, has_side_effects=True),
    )(
        prompt, keep_scale, new_token, w_query, w_forget, w_value, w_outgate,
        floor_gap.reshape(1, width), norm_gain.reshape(1, head),
    )


def solution(mesh):
    return jax.shard_map(
        per_device,
        mesh=mesh,
        in_specs=(
            P(None, "sp", None),
            P(None, "sp"),
            P(None, "tp"),
            P(None, "tp"),
            P(None, "tp"),
            P(None, "tp"),
            P(None, "tp"),
            P("tp"),
            P(),
        ),
        out_specs=(P("tp", "sp", None), P(None, "tp")),
        check_vma=False,
    )
```

```python
import functools

import jax
import jax.numpy as jnp
from jax import lax
from jax.experimental import pallas as pl
from jax.experimental.pallas import tpu as pltpu
from jax.sharding import PartitionSpec as P

EPSILON = 1e-06
MESH = pl.DeviceIdType.MESH
F32 = jnp.float32
BF16 = jnp.bfloat16


def partner(mine, step, count):
    total, bit = 0, 1
    while bit < count:
        total = total + bit * lax.rem(lax.rem(mine // bit, 2) + lax.rem(step // bit, 2), 2)
        bit *= 2
    return total


def pieces(x, count):
    out = []
    for _ in range(count):
        piece = x.astype(BF16)
        out.append(piece)
        x = x - piece.astype(F32)
    return out


def kernel(
    sizes,
    prompt, keep, token, w_query, w_forget, w_value, w_outgate, floor, gain,
    cache_out, read_out,
    blocks, keeps, tokens, wq, wf, wv, wo, weighted, values, logs, totals, got_totals, states, got_states, reads, sums,
    local_sem, direct_send, direct_recv, keep_send, keep_recv, fwd_send, fwd_recv,
    token_send, token_recv, total_send, total_recv, row_send, row_recv, state_send, state_recv, read_send, read_recv,
):
    n, t, s_count, members, group, heads, head, rows = sizes
    planes = n // members
    me, core = lax.axis_index("sp"), lax.axis_index("tp")
    plane, place = me // members, lax.rem(me, members)
    model = prompt.shape[2]
    part = model // t
    positions = prompt.shape[1]
    width = heads * head
    side = 2
    batches = 2 if heads % 2 == 0 else 1
    batch = heads // batches

    def class_of(p):
        return lax.rem(p, side) * (members // side) + p // side

    def member_of(q):
        return (q % (members // side)) * side + q // (members // side)

    def turn(a, z):
        return (1 + a + (2 * z) // planes) % 2

    def prompt_of(p, a):
        return class_of(p) + members * turn(a, plane)

    def columns(c):
        return pl.ds(pl.multiple_of(c * part, part), part)

    def peer(r):
        return partner(place, r, members)

    local = [
        pltpu.make_async_copy(prompt.at[prompt_of(place, 0)], blocks.at[0, place], local_sem.at[0]),
        pltpu.make_async_copy(prompt.at[prompt_of(place, 1)], blocks.at[1, place], local_sem.at[1]),
        pltpu.make_async_copy(w_forget, wf, local_sem.at[2]),
        pltpu.make_async_copy(w_value, wv, local_sem.at[3]),
        pltpu.make_async_copy(w_query, wq, local_sem.at[4]),
        pltpu.make_async_copy(w_outgate, wo, local_sem.at[5]),
    ]

    barrier = pltpu.get_barrier_semaphore()
    for o in range(1, n):
        pl.semaphore_signal(barrier, inc=1, device_id=(lax.rem(me + o, n), core), device_id_type=MESH)
    for o in range(1, t):
        pl.semaphore_signal(barrier, inc=1, device_id=(me, lax.rem(core + o, t)), device_id_type=MESH)
    for copy in local:
        copy.start()
    pl.semaphore_wait(barrier, n - 1 + t - 1)

    def direct(a, r):
        to = peer(r)
        return pltpu.make_async_remote_copy(
            src_ref=prompt.at[prompt_of(to, a), :, columns(core)],
            dst_ref=blocks.at[a, place, :, columns(core)],
            send_sem=direct_send.at[a, r], recv_sem=direct_recv.at[a, r],
            device_id=(plane * members + to, core), device_id_type=MESH,
        )

    def direct_in(a, r):
        frm = peer(r)
        return pltpu.make_async_remote_copy(
            src_ref=prompt.at[prompt_of(frm, a), :, columns(core)],
            dst_ref=blocks.at[a, frm, :, columns(core)],
            send_sem=direct_send.at[a, r], recv_sem=direct_recv.at[a, r],
            device_id=(plane * members + frm, core), device_id_type=MESH,
        )

    def keep_copy(r):
        return pltpu.make_async_remote_copy(
            src_ref=keep, dst_ref=keeps.at[r],
            send_sem=keep_send.at[r], recv_sem=keep_recv.at[r],
            device_id=(plane * members + peer(r), core), device_id_type=MESH,
        )

    def forward(a, r, o, c):
        piece = blocks.at[a, peer(r), :, columns(c)]
        return pltpu.make_async_remote_copy(
            src_ref=piece, dst_ref=piece,
            send_sem=fwd_send.at[a, r, o], recv_sem=fwd_recv.at[a, r, o],
            device_id=(me, lax.rem(core + o, t)), device_id_type=MESH,
        )

    def token_copy(o, c):
        return pltpu.make_async_remote_copy(
            src_ref=token, dst_ref=tokens.at[c],
            send_sem=token_send.at[o], recv_sem=token_recv.at[o],
            device_id=(me, lax.rem(core + o, t)), device_id_type=MESH,
        )

    for r in range(1, members):
        keep_copy(r).start()
    for a in range(2):
        for r in range(1, members):
            direct(a, r).start()
    for o in range(1, t):
        token_copy(o, core).start()

    keeps[0] = keep[...]
    tokens[core] = token[...]
    floor_row = floor[...]

    def value(a, r):
        p = peer(r)
        values[a, p] = jnp.dot(blocks[a, p], wv[...], preferred_element_type=F32).astype(BF16)

    def forget(a, r):
        p = peer(r)
        pre = jnp.dot(blocks[a, p], wf[...], preferred_element_type=F32)
        loss = floor_row * (1.0 / (1.0 + jnp.exp(pre)))
        row = keeps[r, pl.ds(prompt_of(place, a), 1), :]
        i0 = lax.broadcasted_iota(jnp.int32, (positions, positions), 0)
        i1 = lax.broadcasted_iota(jnp.int32, (positions, positions), 1)
        scale = jnp.sum(jnp.where(i0 == i1, jnp.broadcast_to(row, (positions, positions)), 0.0), axis=1, keepdims=True)
        log_forget = jnp.log(scale) + jnp.log1p(-loss)
        gate = 1.0 - scale + scale * loss
        later = jnp.where(i1 > i0, 1.0, 0.0).astype(BF16)
        inside = sum(jnp.dot(later, piece, preferred_element_type=F32) for piece in pieces(log_forget, 3))
        logs[a, pl.ds(p, 1), :] = inside[0:1] + log_forget[0:1]
        weighted[a, p] = gate * jnp.exp(inside)

    def total_copy(k, o, z):
        return pltpu.make_async_remote_copy(
            src_ref=totals.at[k, z], dst_ref=totals.at[k, z],
            send_sem=total_send.at[k, o], recv_sem=total_recv.at[k, o],
            device_id=(lax.rem(me + o * members, n), core), device_id_type=MESH,
        )

    def keeper(a, g):
        return prompt_of(place, a) * group + g

    def row_copy(a, g):
        return pltpu.make_async_remote_copy(
            src_ref=totals.at[turn(a, plane), plane], dst_ref=got_totals.at[plane],
            send_sem=row_send.at[a, g], recv_sem=row_recv.at[plane],
            device_id=(keeper(a, g), core), device_id_type=MESH,
        )

    def state_copy(a, g, b):
        return pltpu.make_async_remote_copy(
            src_ref=states.at[a, pl.ds(b * batch, batch), pl.ds(g * rows, rows), :],
            dst_ref=got_states.at[plane, pl.ds(b * batch, batch)],
            send_sem=state_send.at[a, g, b], recv_sem=state_recv.at[plane, b],
            device_id=(keeper(a, g), core), device_id_type=MESH,
        )

    def read_copy(o, sender):
        return pltpu.make_async_remote_copy(
            src_ref=reads.at[sender], dst_ref=reads.at[sender],
            send_sem=read_send.at[o], recv_sem=read_recv.at[o],
            device_id=(lax.rem(me + o, n), core), device_id_type=MESH,
        )

    def finish(a):
        suffixes, suffix = [None] * members, jnp.zeros((1, width), F32)
        for p in reversed(range(members)):
            suffixes[p] = suffix
            suffix = suffix + logs[a, p : p + 1, :]
        k = turn(a, plane)
        totals[k, plane] = suffix
        for o in range(1, planes):
            total_copy(k, o, plane).start()
        value(a, members - 1)
        for p in range(members):
            weighted[a, p] = weighted[a, p] * jnp.exp(suffixes[p])
        for h in range(heads):
            lanes = slice(h * head, (h + 1) * head)
            w = weighted[a, :, :, lanes].reshape(members * positions, head)
            v = values[a, :, :, lanes].reshape(members * positions, head)
            states[a, h] = sum(
                lax.dot_general(piece, v, (((0,), (0,)), ((), ())), preferred_element_type=F32)
                for piece in pieces(w, 2)
            )
        for g in range(group):

            @pl.when(keeper(a, g) != me)
            def _():
                row_copy(a, g).start()
                for b in range(batches if a == 0 else 1):
                    state_copy(a, g, b).start()

            @pl.when(keeper(a, g) == me)
            def _():
                got_totals[plane] = suffix
                got_states[plane] = states[a, :, g * rows : (g + 1) * rows, :]

    def send_reads():
        for o in range(1, planes):
            z = lax.rem(plane - o + planes, planes)
            for k in range(2):
                total_copy(k, o, z).wait_recv()
        for a in range(2):
            later = jnp.zeros((1, width), F32)
            for z in range(planes):
                later = later + jnp.where(z > plane, totals[turn(a, plane), z], 0.0)
            decay = jnp.exp(later)
            for h in range(heads):
                lanes = slice(h * head, (h + 1) * head)
                reads[me, a, :, lanes] = jnp.dot(
                    sums[3 + a, :, lanes] * decay[:, lanes], states[a, h],
                    preferred_element_type=F32, precision=lax.Precision.HIGHEST,
                )[0:1]
        for o in range(n - 1, 0, -1):
            read_copy(o, me).start()
        for g in range(group):

            @pl.when(keeper(1, g) != me)
            def _():
                for b in range(1, batches):
                    state_copy(1, g, b).start()

    for copy in local[:4]:
        copy.wait()

    def own_block(a, carry):
        forget(a, 0)
        value(a, 0)
        return carry

    lax.fori_loop(0, 2, own_block, 0)

    local[4].wait()
    local[5].wait()
    for o in range(1, t):
        token_copy(o, lax.rem(core - o + t, t)).wait_recv()
    feature = jnp.concatenate([tokens[c] for c in range(t)], axis=1)
    query = jnp.dot(feature, wq[...], preferred_element_type=F32)
    new_forget = jnp.dot(feature, wf[...], preferred_element_type=F32)
    new_value = jnp.dot(feature, wv[...], preferred_element_type=F32).astype(BF16).astype(F32)
    new_gate = jnp.dot(feature, wo[...], preferred_element_type=F32)
    new_loss = floor_row * (1.0 / (1.0 + jnp.exp(new_forget)))
    read_weight = query * (1.0 - new_loss)
    sums[0] = query * new_loss
    sums[1] = new_value
    sums[2] = new_gate * (1.0 / (1.0 + jnp.exp(-new_gate)))
    seq = lax.broadcasted_iota(jnp.int32, read_weight.shape, 0)
    for a in range(2):
        picked = jnp.where(seq == prompt_of(place, a), read_weight, 0.0)
        sums[3 + a] = jnp.broadcast_to(jnp.sum(picked, axis=0, keepdims=True), read_weight.shape)

    def arrive(a, r):
        direct_in(a, r).wait_recv()
        for o in range(1, t):
            forward(a, r, o, core).start()

    def ready(a, r):
        if a == 0:
            keep_copy(r).wait_recv()
        for o in range(1, t):
            forward(a, r, o, lax.rem(core - o + t, t)).wait_recv()

    arrive(0, 1)
    for a in range(2):

        def step(r, carry, a=a):
            arrive(a, r)
            ready(a, r - 1)
            forget(a, r - 1)
            value(a, r - 1)
            return carry

        lax.fori_loop(2, members, step, 0)
        if a == 0:
            arrive(1, 1)
        ready(a, members - 1)
        forget(a, members - 1)
        finish(a)
    send_reads()

    mine = me // group
    source = member_of(lax.rem(mine, members))
    for z in range(planes):

        @pl.when(z * members + source != me)
        def _():
            pairs = [(got_totals.at[z], row_recv.at[z])]
            for b in range(batches):
                pairs.append((got_states.at[z, pl.ds(b * batch, batch)], state_recv.at[z, b]))
            for piece, arrived in pairs:
                pltpu.make_async_remote_copy(
                    src_ref=piece, dst_ref=piece,
                    send_sem=row_send.at[0, 0], recv_sem=arrived,
                    device_id=(z * members + source, core), device_id_type=MESH,
                ).wait_recv()

    first = lax.rem(me, group) * rows
    i0 = lax.broadcasted_iota(jnp.int32, (rows, head), 0) + first
    i1 = lax.broadcasted_iota(jnp.int32, (rows, head), 1)
    later = jnp.zeros((1, width), F32)
    final = [got_states[planes - 1, h] for h in range(heads)]
    for z in reversed(range(planes - 1)):
        later = later + got_totals[z + 1]
        decay = jnp.exp(later)
        for h in range(heads):
            row = jnp.broadcast_to(decay[:, h * head : (h + 1) * head], (rows, head))
            final[h] = final[h] + got_states[z, h] * jnp.sum(jnp.where(i0 == i1, row, 0.0), axis=1, keepdims=True)
    for h in range(heads):
        cache_out[h] = final[h].astype(BF16)

    for o in range(1, n):
        read_copy(o, lax.rem(me - o + n, n)).wait_recv()
    for s in range(s_count):
        row = jnp.zeros((1, width), F32)
        for z in range(planes):
            a = (s // members + 1 + (2 * z) // planes) % 2
            row = row + reads[z * members + member_of(s % members), a]
        sums[5, s : s + 1, :] = row
    for h in range(heads):
        lanes = slice(h * head, (h + 1) * head)
        mixed = sums[5, :, lanes] + jnp.sum(sums[0, :, lanes], axis=1, keepdims=True) * sums[1, :, lanes]
        normed = mixed * lax.rsqrt(jnp.mean(mixed * mixed, axis=1, keepdims=True) + EPSILON)
        read_out[:, lanes] = (normed * gain[...] * sums[2, :, lanes]).astype(BF16)

    for r in range(1, members):
        keep_copy(r).wait_send()
    for o in range(1, t):
        token_copy(o, core).wait_send()
    for a in range(2):
        for r in range(1, members):
            direct(a, r).wait_send()
            for o in range(1, t):
                forward(a, r, o, core).wait_send()
        for o in range(1, planes):
            total_copy(a, o, plane).wait_send()
        for g in range(group):

            @pl.when(keeper(a, g) != me)
            def _():
                row_copy(a, g).wait_send()
                for b in range(batches):
                    state_copy(a, g, b).wait_send()

    for o in range(1, n):
        read_copy(o, me).wait_send()


def per_device(prompt, keep_scale, new_token, w_query, w_forget, w_value, w_outgate, floor_gap, norm_gain):
    n, t = lax.axis_size("sp"), lax.axis_size("tp")
    s_count, positions, model = prompt.shape
    head = norm_gain.shape[0]
    width = w_forget.shape[1]
    heads = width // head
    members = s_count // 2
    planes = n // members
    group = n // s_count
    rows = head // group
    batches = 2 if heads % 2 == 0 else 1
    sizes = (n, t, s_count, members, group, heads, head, rows)
    dma = pltpu.SemaphoreType.DMA
    vmem = pl.BlockSpec(memory_space=pltpu.VMEM)
    hbm = pl.BlockSpec(memory_space=pl.ANY)
    return pl.pallas_call(
        functools.partial(kernel, sizes),
        out_shape=(
            jax.ShapeDtypeStruct((heads, rows, head), BF16),
            jax.ShapeDtypeStruct((s_count, width), BF16),
        ),
        in_specs=[hbm, vmem, vmem, hbm, hbm, hbm, hbm, vmem, vmem],
        out_specs=(vmem, vmem),
        scratch_shapes=[
            pltpu.VMEM((2, members, positions, model), BF16),
            pltpu.VMEM((members,) + keep_scale.shape, F32),
            pltpu.VMEM((t,) + new_token.shape, BF16),
            pltpu.VMEM((model, width), BF16),
            pltpu.VMEM((model, width), BF16),
            pltpu.VMEM((model, width), BF16),
            pltpu.VMEM((model, width), BF16),
            pltpu.VMEM((2, members, positions, width), F32),
            pltpu.VMEM((2, members, positions, width), BF16),
            pltpu.VMEM((2, members, width), F32),
            pltpu.VMEM((2, planes, 1, width), F32),
            pltpu.VMEM((planes, 1, width), F32),
            pltpu.VMEM((2, heads, head, head), F32),
            pltpu.VMEM((planes, heads, rows, head), F32),
            pltpu.VMEM((n, 2, 1, width), F32),
            pltpu.VMEM((6, s_count, width), F32),
            dma((6,)),
            dma((2, members)), dma((2, members)),
            dma((members,)), dma((members,)),
            dma((2, members, t)), dma((2, members, t)),
            dma((t,)), dma((t,)),
            dma((2, planes)), dma((2, planes)),
            dma((2, group)), dma((planes,)),
            dma((2, group, batches)), dma((planes, batches)),
            dma((n,)), dma((n,)),
        ],
        compiler_params=pltpu.CompilerParams(collective_id=0, has_side_effects=True),
    )(
        prompt, keep_scale, new_token, w_query, w_forget, w_value, w_outgate,
        floor_gap.reshape(1, width), norm_gain.reshape(1, head),
    )


def solution(mesh):
    return jax.shard_map(
        per_device,
        mesh=mesh,
        in_specs=(
            P(None, "sp", None),
            P(None, "sp"),
            P(None, "tp"),
            P(None, "tp"),
            P(None, "tp"),
            P(None, "tp"),
            P(None, "tp"),
            P("tp"),
            P(),
        ),
        out_specs=(P("tp", "sp", None), P(None, "tp")),
        check_vma=False,
    )
```
